32 devices in a mesh: fs: 16 (over z, y, core), tp: 2 (over x).
Axes of the slice: x: 2, y: 2, z: 4, core: 2. Of those that a mesh axis runs over, the one named last changes fastest.
Arguments:
- tokens: bfloat16 [16384, 2048], P(('fs', 'tp')), may hold values from -8 to 8
- pre_mix_gain: float32 [2048], replicated, may hold values from 0.1 to 1.9
- post_mix_gain: float32 [2048], replicated, may hold values from 0.1 to 1.9
- pre_ffn_gain: float32 [2048], replicated, may hold values from 0.1 to 1.9
- post_ffn_gain: float32 [2048], replicated, may hold values from 0.1 to 1.9
- w_branch: bfloat16 [2048, 1024], P('fs', 'tp'), may hold values from -0.125 to 0.125
- w_gelu: bfloat16 [2048, 1024], P('fs', 'tp'), may hold values from -0.125 to 0.125
- conv_weight: bfloat16 [4, 1024], P(None, 'tp'), may hold values from -3 to 3
- w_rec: bfloat16 [2, 8, 128, 128], P(None, 'tp'), may hold values from -0.5 to 0.5
- w_inp: bfloat16 [2, 8, 128, 128], P(None, 'tp'), may hold values from -0.5 to 0.5
- decay: float32 [2, 1024], P(None, 'tp'), may hold values from 3 to 10
- out_weight_t: bfloat16 [2048, 1024], P('fs', 'tp'), may hold values from -0.1875 to 0.1875
- w_gate: bfloat16 [2048, 3072], P('fs', 'tp'), may hold values from -0.125 to 0.125
- w_up: bfloat16 [2048, 3072], P('fs', 'tp'), may hold values from -0.125 to 0.125
- down_weight_t: bfloat16 [2048, 3072], P('fs', 'tp'), may hold values from -0.109375 to 0.109375
Outputs:
- layer_out: bfloat16 [16384, 2048], P(('fs', 'tp'))
The draws below stay inside these ranges and needn't reach their ends.
All inputs are finite; a program needn't handle non-finite values.
Results may differ from the reference program's by a relative error of at most 0.014.
Values may be sent and summed in bfloat16 or wider, within the bound.
A program may use at most 128 MiB of HBM per device.

```python
import math
import jax
import jax.numpy as jnp
from jax import lax

D = 2048
BLOCKS = 8
BW = 128
FF = 3072
SEQ_LEN = 1024
D_LRU = 1024
TOKENS = 16384
N_FS = 16
N_TP = 2


def draw_tokens(key, part):
    noise_key = jax.random.fold_in(key, 11)
    common_key = jax.random.fold_in(key, 12)
    block_count = (TOKENS + 15) // 16
    block_index = jnp.arange(TOKENS) // 16
    common = jax.random.normal(common_key, (block_count, D), jnp.float32)
    noise = jax.random.normal(noise_key, (TOKENS, D), jnp.float32)
    values = noise + 1.2 * common[block_index]
    return jnp.clip(values, -8.0, 8.0).astype(jnp.bfloat16)


def draw_decay(key, part):
    choose_key = jax.random.fold_in(key, 21)
    slow_key = jax.random.fold_in(key, 22)
    fast_key = jax.random.fold_in(key, 23)
    fast_share = 0.5
    fast = jax.random.uniform(choose_key, (2, D_LRU), jnp.float32) < fast_share
    slow_rate = jnp.exp(jax.random.uniform(slow_key, (2, D_LRU), jnp.float32, math.log(0.3), math.log(1.5))) / SEQ_LEN
    fast_rate = 1.0 / jnp.exp(jax.random.uniform(fast_key, (2, D_LRU), jnp.float32, math.log(15.0), math.log(50.0)))
    per_step = jnp.where(fast, fast_rate, slow_rate)
    return (-jnp.log(jnp.expm1(per_step / 4.0))).astype(jnp.float32)


def steps_of(rng, shape, cuts, smallest, high):
    level, own = 1.0, jax.random.fold_in(rng, 6)
    for dim, blocks in cuts:
        steps = jnp.exp(jax.random.uniform(jax.random.fold_in(own, dim), (blocks,), jnp.float32, smallest / len(cuts), high / len(cuts)))
        level = level * jnp.repeat(steps, shape[dim] // blocks).reshape([-1 if axis == dim else 1 for axis in range(len(shape))])
    return level


def gaussian(own_key, dims, deviation, reach, split=(), held_as=jnp.bfloat16):
    values = deviation * jax.random.normal(own_key, dims, jnp.float32)
    if split:
        values = values * steps_of(own_key, dims, split, -0.22, 0.18)
    return jnp.clip(values, -reach, reach).astype(held_as)


def setup_inputs(seed: int = 0) -> dict:
    key_list = jax.random.split(jax.random.key(seed), 16)
    return {
        "tokens": draw_tokens(jax.random.fold_in(key_list[15], 71), 0),
        "pre_mix_gain": jnp.clip(1.0 + 0.18 * jax.random.normal(key_list[1], (D,), jnp.float32), 0.1, 1.9),
        "post_mix_gain": jnp.clip(1.0 + 0.18 * jax.random.normal(key_list[2], (D,), jnp.float32), 0.1, 1.9),
        "pre_ffn_gain": jnp.clip(1.0 + 0.18 * jax.random.normal(key_list[3], (D,), jnp.float32), 0.1, 1.9),
        "post_ffn_gain": jnp.clip(1.0 + 0.18 * jax.random.normal(key_list[4], (D,), jnp.float32), 0.1, 1.9),
        "w_branch": gaussian(key_list[5], (D, D_LRU), D ** -0.5, 0.125, ((0, 16), (1, 2))),
        "w_gelu": gaussian(key_list[6], (D, D_LRU), D ** -0.5, 0.125, ((0, 16), (1, 2))),
        "conv_weight": gaussian(key_list[7], (4, D_LRU), 0.5, 3.0, ((1, 2),)),
        "w_rec": gaussian(key_list[8], (2, BLOCKS, BW, BW), BW ** -0.5, 0.5, ((1, 2),)),
        "w_inp": gaussian(key_list[9], (2, BLOCKS, BW, BW), BW ** -0.5, 0.5, ((1, 2),)),
        "decay": draw_decay(jax.random.fold_in(key_list[15], 71), 0),
        "out_weight_t": gaussian(key_list[11], (D, D_LRU), D_LRU ** -0.5, 0.1875, ((0, 16), (1, 2))),
        "w_gate": gaussian(key_list[12], (D, FF), D ** -0.5, 0.125, ((0, 16), (1, 2))),
        "w_up": gaussian(key_list[13], (D, FF), D ** -0.5, 0.125, ((0, 16), (1, 2))),
        "down_weight_t": gaussian(key_list[14], (D, FF), FF ** -0.5, 0.109375, ((0, 16), (1, 2))),
    }


EPS = 1e-06

def normed(values, gain):
    factor = lax.rsqrt(lax.optimization_barrier(jnp.mean(values * values, axis=-1, keepdims=True)) + EPS)
    return values * factor * gain

def conv_short(branch, conv_weight):
    length = branch.shape[0]
    padded = jnp.pad(branch.astype(jnp.float32), ((2, 1), (0, 0)))
    weights = conv_weight.astype(jnp.float32)
    summed = weights[0] * padded[0:length]
    for offset in range(1, 4):
        summed = summed + weights[offset] * padded[offset:offset + length]
    return summed.astype(jnp.bfloat16)

def combine(earlier, later):
    return (earlier[0] * later[0], later[0] * earlier[1] + later[1])

def recurrence(conv_out, w_rec, w_inp, decay):
    length, channels = conv_out.shape
    blocks = w_rec.shape[0]
    grouped = conv_out.astype(jnp.float32).reshape(length, blocks, channels // blocks)
    rate_gate = jax.nn.sigmoid(jnp.einsum('lnc,ncd->lnd', grouped, w_rec.astype(jnp.float32)).reshape(length, channels))
    inflow = jax.nn.sigmoid(jnp.einsum('lnc,ncd->lnd', grouped, w_inp.astype(jnp.float32)).reshape(length, channels))
    log_retain = -8.0 * rate_gate * jax.nn.softplus(-decay)
    retain = jnp.exp(log_retain)
    feed = jnp.sqrt(-jnp.expm1(2.0 * log_retain)) * inflow * conv_out.astype(jnp.float32)
    unused_decay, states = lax.associative_scan(combine, (retain, feed), axis=0)
    return states

def grouped_sum(hidden, weight_t):
    group_cols = hidden.shape[1] // N_TP

    def add_group(index, summed):
        first_col = (index * group_cols).astype(jnp.int32)
        part_rows = lax.dynamic_slice_in_dim(hidden, first_col, group_cols, 1)
        part_cols = lax.dynamic_slice_in_dim(weight_t, first_col, group_cols, 1)
        partial_value = lax.dot_general(part_rows, part_cols, (((1,), (1,)), ((), ())), preferred_element_type=jnp.float32)
        rounded = lax.optimization_barrier(partial_value.astype(jnp.bfloat16))
        return summed + rounded.astype(jnp.float32)
    zero_block = jnp.zeros((hidden.shape[0], weight_t.shape[0]), jnp.float32)
    return lax.fori_loop(0, N_TP, add_group, zero_block)

def reference(tokens, pre_mix_gain, post_mix_gain, pre_ffn_gain, post_ffn_gain, w_branch, w_gelu, conv_weight, w_rec, w_inp, decay, out_weight_t, w_gate, w_up, down_weight_t):

    def one_sequence(seq_tokens):
        stream = seq_tokens.astype(jnp.float32)
        normed_in = normed(stream, pre_mix_gain).astype(jnp.bfloat16)
        branch_in = jnp.dot(normed_in, w_branch, preferred_element_type=jnp.float32).astype(jnp.bfloat16)
        gelu_in = jnp.dot(normed_in, w_gelu, preferred_element_type=jnp.float32).astype(jnp.bfloat16)
        conv_out = conv_short(branch_in, conv_weight)
        forward = recurrence(conv_out, w_rec[0], w_inp[0], decay[0])
        backward = jnp.flip(recurrence(jnp.flip(conv_out, 0), w_rec[1], w_inp[1], decay[1]), 0)
        mixer_hidden = (jax.nn.gelu(gelu_in.astype(jnp.float32)) * (forward + backward)).astype(jnp.bfloat16)
        mixer_sum = lax.dot_general(mixer_hidden, out_weight_t, (((1,), (1,)), ((), ())), preferred_element_type=jnp.float32)
        residual = (stream + normed(mixer_sum, post_mix_gain)).astype(jnp.bfloat16)
        middle = residual.astype(jnp.float32)
        normed_mid = normed(middle, pre_ffn_gain).astype(jnp.bfloat16)
        gate_proj = jnp.dot(normed_mid, w_gate, preferred_element_type=jnp.float32)
        up_proj = jnp.dot(normed_mid, w_up, preferred_element_type=jnp.float32)
        ffn_hidden = (jax.nn.silu(gate_proj) * up_proj).astype(jnp.bfloat16)
        ffn_sum = grouped_sum(ffn_hidden, down_weight_t)
        return (middle + normed(ffn_sum, post_ffn_gain)).astype(jnp.bfloat16)
    sequences = tokens.reshape(N_FS, SEQ_LEN, D)
    outputs = lax.map(one_sequence, sequences)
    return outputs.reshape(N_FS * SEQ_LEN, D)
```

```python
import functools

import jax
import jax.numpy as jnp
from jax import lax
from jax.experimental import pallas as pl
from jax.experimental.pallas import tpu as pltpu
from jax.sharding import PartitionSpec as P

EPS = 1e-06
SEGMENTS = 8
VMEM_BYTES = 60 * 1024 * 1024


def normed(values, gain):
    factor = lax.rsqrt(jnp.mean(values * values, axis=-1, keepdims=True) + EPS)
    return values * factor * gain


def one_minus_exp(y, exp_y):
    series = 1.0 + y * (1.0 / 8.0)
    for order in (7, 6, 5, 4, 3, 2):
        series = 1.0 + y * (1.0 / order) * series
    return jnp.where(y > -0.5, -y * series, 1.0 - exp_y)


def mixer_kernel(
    x_ref, wb_ref, wg_ref, conv_ref, gates_ref, coef_ref, out_ref, pad, gel, a0, u0, a1, u1
):
    length, width = out_ref.shape
    group = gates_ref.shape[1]
    rows = 256
    pad[0:8, :] = jnp.zeros((8, width), jnp.float32)
    pad[8 + length : 16 + length, :] = jnp.zeros((8, width), jnp.float32)
    for start in range(0, length, rows):
        piece = x_ref[start : start + rows, :]
        branch = jnp.dot(piece, wb_ref[...], preferred_element_type=jnp.float32)
        pad[8 + start : 8 + start + rows, :] = branch.astype(jnp.bfloat16).astype(jnp.float32)
        gelu_in = jnp.dot(piece, wg_ref[...], preferred_element_type=jnp.float32)
        gel[start : start + rows, :] = jax.nn.gelu(
            gelu_in.astype(jnp.bfloat16).astype(jnp.float32)
        )

    for part in range(width // group):
        cols = slice(part * group, (part + 1) * group)
        taps = conv_ref[:, cols].astype(jnp.float32)
        coef = coef_ref[:, cols]
        for start in range(0, length, rows):
            summed = taps[0:1] * pad[6 + start : 6 + start + rows, cols]
            for j in range(1, 4):
                summed = summed + taps[j : j + 1] * pad[6 + j + start : 6 + j + start + rows, cols]
            conv = summed.astype(jnp.bfloat16)
            wide = conv.astype(jnp.float32)
            for d, (a_ref, u_ref) in enumerate(((a0, u0), (a1, u1))):
                gate = jnp.dot(
                    conv,
                    gates_ref[part, :, 2 * d * group : 2 * (d + 1) * group],
                    preferred_element_type=jnp.float32,
                )
                rate = jax.nn.sigmoid(gate[:, :group])
                inflow = jax.nn.sigmoid(gate[:, group:])
                log_retain = rate * coef[d : d + 1]
                retain = jnp.exp(log_retain)
                left = one_minus_exp(2.0 * log_retain, retain * retain)
                a_ref[part, start : start + rows, :] = retain
                u_ref[part, start : start + rows, :] = jnp.sqrt(left) * inflow * wide

    steps = length // SEGMENTS

    def step(t, carry):
        out = []
        for (state, decayed), (a_ref, u_ref), at in (
            (carry[0], (a0, u0), t),
            (carry[1], (a1, u1), steps - 1 - t),
        ):
            where = pl.ds(at, SEGMENTS, stride=steps)
            nstate, ndecayed = [], []
            for c in range(n):
                retain = a_ref[c, where, :]
                h = retain * state[c] + u_ref[c, where, :]
                p = retain * decayed[c]
                u_ref[c, where, :] = h
                a_ref[c, where, :] = p
                nstate.append(h)
                ndecayed.append(p)
            out.append((tuple(nstate), tuple(ndecayed)))
        return tuple(out)

    n = width // group
    zero = tuple(jnp.zeros((SEGMENTS, group), jnp.float32) for c in range(n))
    one = tuple(jnp.ones((SEGMENTS, group), jnp.float32) for c in range(n))
    ended = lax.fori_loop(0, steps, step, ((zero, one), (zero, one)), unroll=8)
    for c in range(n):
        lanes = slice(c * group, (c + 1) * group)
        blank = jnp.zeros((1, group), jnp.float32)
        entry = [[None] * SEGMENTS, [None] * SEGMENTS]
        for d, order in ((0, range(SEGMENTS)), (1, range(SEGMENTS - 1, -1, -1))):
            carry = blank
            for s in order:
                entry[d][s] = carry
                carry = ended[d][0][c][s : s + 1] + ended[d][1][c][s : s + 1] * carry
        for s in range(SEGMENTS):
            span = slice(s * steps, (s + 1) * steps)
            forward = u0[c, span, :] + a0[c, span, :] * entry[0][s]
            backward = u1[c, span, :] + a1[c, span, :] * entry[1][s]
            out_ref[span, lanes] = (gel[span, lanes] * (forward + backward)).astype(jnp.bfloat16)


def mixer(x, weights, conv_weight, w_rec, w_inp, decay):
    length, model = x.shape
    channels = conv_weight.shape[1]
    group = w_rec.shape[2]
    width = min(256, channels)
    count = channels // width
    gates = jnp.concatenate([w_rec[0], w_inp[0], w_rec[1], w_inp[1]], axis=-1)
    coef = -8.0 * jax.nn.softplus(-decay)
    f32 = functools.partial(pltpu.VMEM, dtype=jnp.float32)
    return pl.pallas_call(
        mixer_kernel,
        grid=(count,),
        out_shape=jax.ShapeDtypeStruct((length, channels), jnp.bfloat16),
        in_specs=[
            pl.BlockSpec((length, model), lambda j: (0, 0)),
            pl.BlockSpec((model, width), lambda j: (0, j)),
            pl.BlockSpec((model, width), lambda j: (0, count + j)),
            pl.BlockSpec((4, width), lambda j: (0, j)),
            pl.BlockSpec((width // group, group, 4 * group), lambda j: (j, 0, 0)),
            pl.BlockSpec((2, width), lambda j: (0, j)),
        ],
        out_specs=pl.BlockSpec((length, width), lambda j: (0, j)),
        scratch_shapes=[f32((length + 16, width)), f32((length, width))]
        + [f32((width // group, length, group)) for i in range(4)],
        compiler_params=pltpu.CompilerParams(vmem_limit_bytes=VMEM_BYTES),
        cost_estimate=pl.CostEstimate(
            flops=4 * length * model * channels + 16 * length * group * channels * 8,
            bytes_accessed=2 * (length * model + 2 * model * channels + length * channels),
            transcendentals=12 * length * channels,
        ),
    )(x, weights, weights, conv_weight, gates, coef)


def ffn_kernel(x_ref, gate_ref, up_ref, down_ref, out_ref, total):
    step = pl.program_id(0)
    gate = jnp.dot(x_ref[...], gate_ref[...], preferred_element_type=jnp.float32)
    up = jnp.dot(x_ref[...], up_ref[...], preferred_element_type=jnp.float32)
    hidden = (jax.nn.silu(gate) * up).astype(jnp.bfloat16)
    partial = lax.dot_general(
        hidden, down_ref[...], (((1,), (1,)), ((), ())), preferred_element_type=jnp.float32
    )

    @pl.when(step == 0)
    def _():
        total[...] = partial

    @pl.when(step > 0)
    def _():
        total[...] += partial

    @pl.when(step == pl.num_programs(0) - 1)
    def _():
        out_ref[...] = total[...].astype(jnp.bfloat16)


def ffn(x, weights):
    rows, model = x.shape
    units = weights.shape[1] // 3
    width = 256 if units % 256 == 0 else 128
    count = units // width
    return pl.pallas_call(
        ffn_kernel,
        grid=(count,),
        out_shape=jax.ShapeDtypeStruct((rows, model), jnp.bfloat16),
        in_specs=[
            pl.BlockSpec((rows, model), lambda j: (0, 0)),
            pl.BlockSpec((model, width), lambda j: (0, j)),
            pl.BlockSpec((model, width), lambda j: (0, count + j)),
            pl.BlockSpec((model, width), lambda j: (0, 2 * count + j)),
        ],
        out_specs=pl.BlockSpec((rows, model), lambda j: (0, 0)),
        scratch_shapes=[pltpu.VMEM((rows, model), jnp.float32)],
        compiler_params=pltpu.CompilerParams(vmem_limit_bytes=VMEM_BYTES),
        cost_estimate=pl.CostEstimate(
            flops=6 * rows * model * units,
            bytes_accessed=2 * (2 * rows * model + 3 * model * units),
            transcendentals=rows * units,
        ),
    )(x, weights, weights, weights)


def swap(values):
    return lax.ppermute(values, "tp", [(0, 1), (1, 0)])


def matmul_t(rows, weight_t):
    return lax.dot_general(
        rows, weight_t, (((1,), (1,)), ((), ())), preferred_element_type=jnp.float32
    )


def per_device(
    pair,
    tokens,
    pre_mix_gain,
    post_mix_gain,
    pre_ffn_gain,
    post_ffn_gain,
    w_branch,
    w_gelu,
    conv_weight,
    w_rec,
    w_inp,
    decay,
    out_weight_t,
    w_gate,
    w_up,
    down_weight_t,
):
    own_rows = tokens.shape[0]
    channels = conv_weight.shape[1]
    place = lax.axis_index("tp")
    parts = [w_branch, w_gelu, out_weight_t]
    if pair:
        parts.append(swap(out_weight_t))
    mix_all = lax.all_gather(jnp.concatenate(parts, axis=1), "fs", axis=0, tiled=True)
    ffn_all = lax.all_gather(
        jnp.concatenate([w_gate, w_up, down_weight_t], axis=1), "fs", axis=0, tiled=True
    )
    stream = tokens.astype(jnp.float32)
    normed_in = normed(stream, pre_mix_gain).astype(jnp.bfloat16)
    if pair:
        other = swap(normed_in)
        first = jnp.where(place == 0, normed_in, other)
        second = jnp.where(place == 0, other, normed_in)
        sequence = jnp.concatenate([first, second], axis=0)
    else:
        sequence = lax.all_gather(normed_in, "tp", axis=0, tiled=True)
    hidden = mixer(sequence, mix_all, conv_weight, w_rec, w_inp, decay)
    out_own = mix_all[:, 2 * channels : 3 * channels]
    if pair:
        away = lax.dynamic_slice_in_dim(hidden, (1 - place) * own_rows, own_rows, 0)
        kept = lax.dynamic_slice_in_dim(hidden, place * own_rows, own_rows, 0)
        came = swap(away)
        mixer_sum = matmul_t(kept, out_own) + matmul_t(came, mix_all[:, 3 * channels :])
    else:
        own_hidden = lax.all_to_all(hidden, "tp", split_axis=0, concat_axis=1, tiled=True)
        out_whole = lax.all_gather(out_own, "tp", axis=1, tiled=True)
        mixer_sum = matmul_t(own_hidden, out_whole)
    residual = (stream + normed(mixer_sum, post_mix_gain)).astype(jnp.bfloat16)
    middle = residual.astype(jnp.float32)
    normed_mid = normed(middle, pre_ffn_gain).astype(jnp.bfloat16)
    if pair:
        pieces = 2
        size = own_rows // pieces
        sums = []
        away_rows = [swap(normed_mid[i * size : (i + 1) * size]) for i in range(pieces)]
        back = [swap(ffn(rows, ffn_all)) for rows in away_rows]
        own_part = ffn(normed_mid, ffn_all).astype(jnp.float32)
        ffn_sum = own_part + jnp.concatenate(back, axis=0).astype(jnp.float32)
    else:
        all_mid = lax.all_gather(normed_mid, "tp", axis=0, tiled=True)
        ffn_sum = lax.psum_scatter(
            ffn(all_mid, ffn_all), "tp", scatter_dimension=0, tiled=True
        ).astype(jnp.float32)
    return (middle + normed(ffn_sum, post_ffn_gain)).astype(jnp.bfloat16)


def solution(mesh):
    return jax.shard_map(
        functools.partial(per_device, mesh.shape["tp"] == 2),
        mesh=mesh,
        in_specs=(
            P(("fs", "tp"), None),
            P(),
            P(),
            P(),
            P(),
            P("fs", "tp"),
            P("fs", "tp"),
            P(None, "tp"),
            P(None, "tp", None, None),
            P(None, "tp", None, None),
            P(None, "tp"),
            P("fs", "tp"),
            P("fs", "tp"),
            P("fs", "tp"),
            P("fs", "tp"),
        ),
        out_specs=P(("fs", "tp"), None),
        check_vma=False,
    )
```

```python
import functools

import jax
import jax.numpy as jnp
from jax import lax
from jax.experimental import pallas as pl
from jax.experimental.pallas import tpu as pltpu
from jax.sharding import PartitionSpec as P

EPS = 1e-06
SEGMENTS = 8
VMEM_BYTES = 60 * 1024 * 1024


def normed(values, gain):
    factor = lax.rsqrt(jnp.mean(values * values, axis=-1, keepdims=True) + EPS)
    return values * factor * gain


def one_minus_exp(y, exp_y):
    series = 1.0 + y * (1.0 / 8.0)
    for order in (7, 6, 5, 4, 3, 2):
        series = 1.0 + y * (1.0 / order) * series
    return jnp.where(y > -0.5, -y * series, 1.0 - exp_y)


def mixer_kernel(
    x_ref, wb_ref, wg_ref, conv_ref, gates_ref, coef_ref, out_ref, pad, gel, a0, u0, a1, u1
):
    length, width = out_ref.shape
    group = gates_ref.shape[1]
    rows = 256
    pad[0:8, :] = jnp.zeros((8, width), jnp.float32)
    pad[8 + length : 16 + length, :] = jnp.zeros((8, width), jnp.float32)
    for start in range(0, length, rows):
        piece = x_ref[start : start + rows, :]
        branch = jnp.dot(piece, wb_ref[...], preferred_element_type=jnp.float32)
        pad[8 + start : 8 + start + rows, :] = branch.astype(jnp.bfloat16).astype(jnp.float32)
        gelu_in = jnp.dot(piece, wg_ref[...], preferred_element_type=jnp.float32)
        gel[start : start + rows, :] = jax.nn.gelu(
            gelu_in.astype(jnp.bfloat16).astype(jnp.float32)
        )

    for part in range(width // group):
        cols = slice(part * group, (part + 1) * group)
        taps = conv_ref[:, cols].astype(jnp.float32)
        coef = coef_ref[:, cols]
        for start in range(0, length, rows):
            summed = taps[0:1] * pad[6 + start : 6 + start + rows, cols]
            for j in range(1, 4):
                summed = summed + taps[j : j + 1] * pad[6 + j + start : 6 + j + start + rows, cols]
            conv = summed.astype(jnp.bfloat16)
            wide = conv.astype(jnp.float32)
            for d, (a_ref, u_ref) in enumerate(((a0, u0), (a1, u1))):
                gate = jnp.dot(
                    conv,
                    gates_ref[part, :, 2 * d * group : 2 * (d + 1) * group],
                    preferred_element_type=jnp.float32,
                )
                rate = jax.nn.sigmoid(gate[:, :group])
                inflow = jax.nn.sigmoid(gate[:, group:])
                log_retain = rate * coef[d : d + 1]
                retain = jnp.exp(log_retain)
                left = one_minus_exp(2.0 * log_retain, retain * retain)
                a_ref[part, start : start + rows, :] = retain
                u_ref[part, start : start + rows, :] = jnp.sqrt(left) * inflow * wide

    steps = length // SEGMENTS

    def step(t, carry):
        out = []
        for (state, decayed), (a_ref, u_ref), at in (
            (carry[0], (a0, u0), t),
            (carry[1], (a1, u1), steps - 1 - t),
        ):
            where = pl.ds(at, SEGMENTS, stride=steps)
            nstate, ndecayed = [], []
            for c in range(n):
                retain = a_ref[c, where, :]
                h = retain * state[c] + u_ref[c, where, :]
                p = retain * decayed[c]
                u_ref[c, where, :] = h
                a_ref[c, where, :] = p
                nstate.append(h)
                ndecayed.append(p)
            out.append((tuple(nstate), tuple(ndecayed)))
        return tuple(out)

    n = width // group
    zero = tuple(jnp.zeros((SEGMENTS, group), jnp.float32) for c in range(n))
    one = tuple(jnp.ones((SEGMENTS, group), jnp.float32) for c in range(n))
    ended = lax.fori_loop(0, steps, step, ((zero, one), (zero, one)), unroll=8)
    for c in range(n):
        lanes = slice(c * group, (c + 1) * group)
        blank = jnp.zeros((1, group), jnp.float32)
        entry = [[None] * SEGMENTS, [None] * SEGMENTS]
        for d, order in ((0, range(SEGMENTS)), (1, range(SEGMENTS - 1, -1, -1))):
            carry = blank
            for s in order:
                entry[d][s] = carry
                carry = ended[d][0][c][s : s + 1] + ended[d][1][c][s : s + 1] * carry
        for s in range(SEGMENTS):
            span = slice(s * steps, (s + 1) * steps)
            forward = u0[c, span, :] + a0[c, span, :] * entry[0][s]
            backward = u1[c, span, :] + a1[c, span, :] * entry[1][s]
            out_ref[span, lanes] = (gel[span, lanes] * (forward + backward)).astype(jnp.bfloat16)


def mixer(x, weights, conv_weight, w_rec, w_inp, decay):
    length, model = x.shape
    channels = conv_weight.shape[1]
    group = w_rec.shape[2]
    width = min(256, channels)
    count = channels // width
    gates = jnp.concatenate([w_rec[0], w_inp[0], w_rec[1], w_inp[1]], axis=-1)
    coef = -8.0 * jax.nn.softplus(-decay)
    f32 = functools.partial(pltpu.VMEM, dtype=jnp.float32)
    return pl.pallas_call(
        mixer_kernel,
        grid=(count,),
        out_shape=jax.ShapeDtypeStruct((length, channels), jnp.bfloat16),
        in_specs=[
            pl.BlockSpec((length, model), lambda j: (0, 0)),
            pl.BlockSpec((model, width), lambda j: (0, j)),
            pl.BlockSpec((model, width), lambda j: (0, count + j)),
            pl.BlockSpec((4, width), lambda j: (0, j)),
            pl.BlockSpec((width // group, group, 4 * group), lambda j: (j, 0, 0)),
            pl.BlockSpec((2, width), lambda j: (0, j)),
        ],
        out_specs=pl.BlockSpec((length, width), lambda j: (0, j)),
        scratch_shapes=[f32((length + 16, width)), f32((length, width))]
        + [f32((width // group, length, group)) for i in range(4)],
        compiler_params=pltpu.CompilerParams(vmem_limit_bytes=VMEM_BYTES),
        cost_estimate=pl.CostEstimate(
            flops=4 * length * model * channels + 16 * length * group * channels * 8,
            bytes_accessed=2 * (length * model + 2 * model * channels + length * channels),
            transcendentals=12 * length * channels,
        ),
    )(x, weights, weights, conv_weight, gates, coef)


def ffn_kernel(x_ref, gate_ref, up_ref, down_ref, out_ref, total):
    step = pl.program_id(0)
    gate = jnp.dot(x_ref[...], gate_ref[...], preferred_element_type=jnp.float32)
    up = jnp.dot(x_ref[...], up_ref[...], preferred_element_type=jnp.float32)
    hidden = (jax.nn.silu(gate) * up).astype(jnp.bfloat16)
    partial = lax.dot_general(
        hidden, down_ref[...], (((1,), (1,)), ((), ())), preferred_element_type=jnp.float32
    )

    @pl.when(step == 0)
    def _():
        total[...] = partial

    @pl.when(step > 0)
    def _():
        total[...] += partial

    @pl.when(step == pl.num_programs(0) - 1)
    def _():
        out_ref[...] = total[...].astype(jnp.bfloat16)


def ffn(x, weights):
    rows, model = x.shape
    units = weights.shape[1] // 3
    width = 256 if units % 256 == 0 else 128
    count = units // width
    return pl.pallas_call(
        ffn_kernel,
        grid=(count,),
        out_shape=jax.ShapeDtypeStruct((rows, model), jnp.bfloat16),
        in_specs=[
            pl.BlockSpec((rows, model), lambda j: (0, 0)),
            pl.BlockSpec((model, width), lambda j: (0, j)),
            pl.BlockSpec((model, width), lambda j: (0, count + j)),
            pl.BlockSpec((model, width), lambda j: (0, 2 * count + j)),
        ],
        out_specs=pl.BlockSpec((rows, model), lambda j: (0, 0)),
        scratch_shapes=[pltpu.VMEM((rows, model), jnp.float32)],
        compiler_params=pltpu.CompilerParams(vmem_limit_bytes=VMEM_BYTES),
        cost_estimate=pl.CostEstimate(
            flops=6 * rows * model * units,
            bytes_accessed=2 * (2 * rows * model + 3 * model * units),
            transcendentals=rows * units,
        ),
    )(x, weights, weights, weights)


def ring_chip(place, chips):
    half = chips // 2
    turned = place // half
    row = place * (1 - turned) + (chips - 1 - place) * turned
    return row * 2 + turned


def ring_kernel(
    size, shard_ref, x_ref, out_ref, seq_ref, own_sem, send, recv, near_send, near_recv, swap_sem
):
    chips = size // 2
    me = lax.axis_index("fs")
    core = me % 2
    turned = (me // 2) % 2
    row = me // 4
    place = row * (1 - turned) + (chips - 1 - row) * turned
    partner = me + 1 - 2 * core
    after = ring_chip((place + 1) % chips, chips) * 2 + core
    before = ring_chip((place + chips - 1) % chips, chips) * 2 + core
    targets = ({"fs": after}, {"fs": before})
    partner = {"fs": partner}
    column = lax.axis_index("tp")
    across = {"tp": 1 - column}

    barrier = pltpu.get_barrier_semaphore()
    for device in (*targets, partner, across):
        pl.semaphore_signal(
            barrier, inc=1, device_id=device, device_id_type=pl.DeviceIdType.MESH
        )
    pl.semaphore_wait(barrier, 4)

    depth = shard_ref.shape[0]
    half = depth // 2

    def remote(src, dst, sent, landed, device):
        copy = pltpu.make_async_remote_copy(
            src_ref=src,
            dst_ref=dst,
            send_sem=sent,
            recv_sem=landed,
            device_id=device,
            device_id_type=pl.DeviceIdType.MESH,
        )
        copy.start()
        return copy

    def rows_of(origin, side):
        start = pl.multiple_of(origin * depth + side * half, half)
        return out_ref.at[pl.ds(start, half), :]

    moving = []
    for side in range(2):
        moving.append(
            remote(
                shard_ref.at[pl.ds(side * half, half), :],
                rows_of(me, side),
                send.at[side, 0],
                recv.at[side, 0],
                targets[side],
            )
        )
    waiting = list(moving)
    count = x_ref.shape[0]
    own_rows = seq_ref.at[pl.ds(pl.multiple_of(column * count, count), count), :]
    near = [remote(x_ref, own_rows, swap_sem.at[0], swap_sem.at[1], across)]
    mine = out_ref.at[pl.ds(pl.multiple_of(me * depth, depth), depth), :]
    near.append(remote(shard_ref, mine, near_send.at[0, 0], near_recv.at[0, 0], partner))
    own = pltpu.make_async_copy(shard_ref, mine, own_sem.at[0])
    own.start()
    kept = pltpu.make_async_copy(x_ref, own_rows, own_sem.at[1])
    kept.start()
    for step in range(chips - 1):
        for side in range(2):
            moving[side].wait_recv()
            back = step + 1 if side == 0 else chips - 1 - step
            origin = ring_chip((place + chips - back) % chips, chips) * 2 + core
            piece = rows_of(origin, side)
            if step < chips - 2:
                moving[side] = remote(
                    piece,
                    piece,
                    send.at[side, step + 1],
                    recv.at[side, step + 1],
                    targets[side],
                )
                waiting.append(moving[side])
            near.append(
                remote(
                    piece,
                    piece,
                    near_send.at[side, step + 1],
                    near_recv.at[side, step + 1],
                    partner,
                )
            )
    for copy in waiting:
        copy.wait_send()
    for copy in near:
        copy.wait()
    own.wait()
    kept.wait()


def ring_gather(shard, x, size):
    rows, width = shard.shape
    chips = size // 2
    dma = pltpu.SemaphoreType.DMA
    return pl.pallas_call(
        functools.partial(ring_kernel, size),
        out_shape=(
            jax.ShapeDtypeStruct((rows * size, width), shard.dtype),
            jax.ShapeDtypeStruct((2 * x.shape[0], x.shape[1]), x.dtype),
        ),
        in_specs=[pl.BlockSpec(memory_space=pl.ANY)] * 2,
        out_specs=(pl.BlockSpec(memory_space=pl.ANY), pl.BlockSpec(memory_space=pl.ANY)),
        scratch_shapes=[
            dma((2,)),
            dma((2, chips)),
            dma((2, chips)),
            dma((2, chips)),
            dma((2, chips)),
            dma((2,)),
        ],
        compiler_params=pltpu.CompilerParams(collective_id=0, has_side_effects=True),
        cost_estimate=pl.CostEstimate(
            flops=1 << 32, bytes_accessed=2 * rows * size * width, transcendentals=0
        ),
    )(shard, x)


def swap(values):
    return lax.ppermute(values, "tp", [(0, 1), (1, 0)])


def matmul_t(rows, weight_t):
    return lax.dot_general(
        rows, weight_t, (((1,), (1,)), ((), ())), preferred_element_type=jnp.float32
    )


def per_device(
    pair,
    tokens,
    pre_mix_gain,
    post_mix_gain,
    pre_ffn_gain,
    post_ffn_gain,
    w_branch,
    w_gelu,
    conv_weight,
    w_rec,
    w_inp,
    decay,
    out_weight_t,
    w_gate,
    w_up,
    down_weight_t,
):
    own_rows = tokens.shape[0]
    channels = conv_weight.shape[1]
    place = lax.axis_index("tp")
    parts = [w_branch, w_gelu, out_weight_t]
    if pair:
        parts.append(swap(out_weight_t))
    mix_shard = jnp.concatenate(parts, axis=1)
    ffn_shard = jnp.concatenate([w_gate, w_up, down_weight_t], axis=1)
    stream = tokens.astype(jnp.float32)
    normed_in = normed(stream, pre_mix_gain).astype(jnp.bfloat16)
    if pair:
        mix_all, sequence = ring_gather(mix_shard, normed_in, lax.axis_size("fs"))
        ffn_shard, mix_all = lax.optimization_barrier((ffn_shard, mix_all))
    else:
        mix_all = lax.all_gather(mix_shard, "fs", axis=0, tiled=True)
        sequence = lax.all_gather(normed_in, "tp", axis=0, tiled=True)
    ffn_all = lax.all_gather(ffn_shard, "fs", axis=0, tiled=True)
    hidden = mixer(sequence, mix_all, conv_weight, w_rec, w_inp, decay)
    out_own = mix_all[:, 2 * channels : 3 * channels]
    if pair:
        away = lax.dynamic_slice_in_dim(hidden, (1 - place) * own_rows, own_rows, 0)
        kept = lax.dynamic_slice_in_dim(hidden, place * own_rows, own_rows, 0)
        came = swap(away)
        mixer_sum = matmul_t(kept, out_own) + matmul_t(came, mix_all[:, 3 * channels :])
    else:
        own_hidden = lax.all_to_all(hidden, "tp", split_axis=0, concat_axis=1, tiled=True)
        out_whole = lax.all_gather(out_own, "tp", axis=1, tiled=True)
        mixer_sum = matmul_t(own_hidden, out_whole)
    residual = (stream + normed(mixer_sum, post_mix_gain)).astype(jnp.bfloat16)
    middle = residual.astype(jnp.float32)
    normed_mid = normed(middle, pre_ffn_gain).astype(jnp.bfloat16)
    if pair:
        pieces = 2
        size = own_rows // pieces
        sums = []
        away_rows = [swap(normed_mid[i * size : (i + 1) * size]) for i in range(pieces)]
        back = [swap(ffn(rows, ffn_all)) for rows in away_rows]
        own_part = ffn(normed_mid, ffn_all).astype(jnp.float32)
        ffn_sum = own_part + jnp.concatenate(back, axis=0).astype(jnp.float32)
    else:
        all_mid = lax.all_gather(normed_mid, "tp", axis=0, tiled=True)
        ffn_sum = lax.psum_scatter(
            ffn(all_mid, ffn_all), "tp", scatter_dimension=0, tiled=True
        ).astype(jnp.float32)
    return (middle + normed(ffn_sum, post_ffn_gain)).astype(jnp.bfloat16)


def solution(mesh):
    return jax.shard_map(
        functools.partial(per_device, mesh.shape["tp"] == 2),
        mesh=mesh,
        in_specs=(
            P(("fs", "tp"), None),
            P(),
            P(),
            P(),
            P(),
            P("fs", "tp"),
            P("fs", "tp"),
            P(None, "tp"),
            P(None, "tp", None, None),
            P(None, "tp", None, None),
            P(None, "tp"),
            P("fs", "tp"),
            P("fs", "tp"),
            P("fs", "tp"),
            P("fs", "tp"),
        ),
        out_specs=P(("fs", "tp"), None),
        check_vma=False,
    )
```

```python
import functools

import jax
import jax.numpy as jnp
from jax import lax
from jax.experimental import pallas as pl
from jax.experimental.pallas import tpu as pltpu
from jax.sharding import PartitionSpec as P

EPS = 1e-06
SEGMENTS = 8
PIECES = 4
VMEM_BYTES = 60 * 1024 * 1024


def normed(values, gain):
    factor = lax.rsqrt(jnp.mean(values * values, axis=-1, keepdims=True) + EPS)
    return values * factor * gain


def one_minus_exp(y, exp_y):
    series = 1.0 + y * (1.0 / 8.0)
    for order in (7, 6, 5, 4, 3, 2):
        series = 1.0 + y * (1.0 / order) * series
    return jnp.where(y > -0.5, -y * series, 1.0 - exp_y)


def mixer_kernel(
    paired, x_ref, y_ref, wb_ref, wg_ref, conv_ref, gates_ref, coef_ref, out_ref, pad, gel, a0, u0, a1, u1
):
    length, width = out_ref.shape
    group = gates_ref.shape[1]
    rows = 256
    pad[0:8, :] = jnp.zeros((8, width), jnp.float32)
    pad[8 + length : 16 + length, :] = jnp.zeros((8, width), jnp.float32)
    if paired:
        own_start = lax.axis_index("tp") * x_ref.shape[0]
        sources = ((x_ref, own_start), (y_ref, x_ref.shape[0] - own_start))
    else:
        sources = ((x_ref, 0),)
    for source, base in sources:
        for start in range(0, source.shape[0], rows):
            piece = source[start : start + rows, :]
            branch = jnp.dot(piece, wb_ref[...], preferred_element_type=jnp.float32)
            gelu_in = jnp.dot(piece, wg_ref[...], preferred_element_type=jnp.float32)
            at = pl.multiple_of(base + start, rows)
            pad[pl.ds(8 + at, rows), :] = branch.astype(jnp.bfloat16).astype(jnp.float32)
            gel[pl.ds(at, rows), :] = jax.nn.gelu(
                gelu_in.astype(jnp.bfloat16).astype(jnp.float32)
            )

    for part in range(width // group):
        cols = slice(part * group, (part + 1) * group)
        taps = conv_ref[:, cols].astype(jnp.float32)
        coef = coef_ref[:, cols]
        for start in range(0, length, rows):
            summed = taps[0:1] * pad[6 + start : 6 + start + rows, cols]
            for j in range(1, 4):
                summed = summed + taps[j : j + 1] * pad[6 + j + start : 6 + j + start + rows, cols]
            conv = summed.astype(jnp.bfloat16)
            wide = conv.astype(jnp.float32)
            for d, (a_ref, u_ref) in enumerate(((a0, u0), (a1, u1))):
                gate = jnp.dot(
                    conv,
                    gates_ref[part, :, 2 * d * group : 2 * (d + 1) * group],
                    preferred_element_type=jnp.float32,
                )
                rate = jax.nn.sigmoid(gate[:, :group])
                inflow = jax.nn.sigmoid(gate[:, group:])
                log_retain = rate * coef[d : d + 1]
                retain = jnp.exp(log_retain)
                left = one_minus_exp(2.0 * log_retain, retain * retain)
                a_ref[part, start : start + rows, :] = retain
                u_ref[part, start : start + rows, :] = jnp.sqrt(left) * inflow * wide

    steps = length // SEGMENTS

    def step(t, carry):
        out = []
        for (state, decayed), (a_ref, u_ref), at in (
            (carry[0], (a0, u0), t),
            (carry[1], (a1, u1), steps - 1 - t),
        ):
            where = pl.ds(at, SEGMENTS, stride=steps)
            nstate, ndecayed = [], []
            for c in range(n):
                retain = a_ref[c, where, :]
                h = retain * state[c] + u_ref[c, where, :]
                p = retain * decayed[c]
                u_ref[c, where, :] = h
                a_ref[c, where, :] = p
                nstate.append(h)
                ndecayed.append(p)
            out.append((tuple(nstate), tuple(ndecayed)))
        return tuple(out)

    n = width // group
    zero = tuple(jnp.zeros((SEGMENTS, group), jnp.float32) for c in range(n))
    one = tuple(jnp.ones((SEGMENTS, group), jnp.float32) for c in range(n))
    ended = lax.fori_loop(0, steps, step, ((zero, one), (zero, one)), unroll=8)
    for c in range(n):
        lanes = slice(c * group, (c + 1) * group)
        blank = jnp.zeros((1, group), jnp.float32)
        entry = [[None] * SEGMENTS, [None] * SEGMENTS]
        for d, order in ((0, range(SEGMENTS)), (1, range(SEGMENTS - 1, -1, -1))):
            carry = blank
            for s in order:
                entry[d][s] = carry
                carry = ended[d][0][c][s : s + 1] + ended[d][1][c][s : s + 1] * carry
        for s in range(SEGMENTS):
            span = slice(s * steps, (s + 1) * steps)
            forward = u0[c, span, :] + a0[c, span, :] * entry[0][s]
            backward = u1[c, span, :] + a1[c, span, :] * entry[1][s]
            out_ref[span, lanes] = (gel[span, lanes] * (forward + backward)).astype(jnp.bfloat16)


def mixer(paired, x, y, weights, conv_weight, w_rec, w_inp, decay):
    length, model = x.shape
    x_spec = pl.BlockSpec((length, model), lambda j: (0, 0))
    length = 2 * length if paired else length
    channels = conv_weight.shape[1]
    group = w_rec.shape[2]
    width = min(256, channels)
    count = channels // width
    gates = jnp.concatenate([w_rec[0], w_inp[0], w_rec[1], w_inp[1]], axis=-1)
    coef = -8.0 * jax.nn.softplus(-decay)
    f32 = functools.partial(pltpu.VMEM, dtype=jnp.float32)
    return pl.pallas_call(
        functools.partial(mixer_kernel, paired),
        grid=(count,),
        out_shape=jax.ShapeDtypeStruct((length, channels), jnp.bfloat16),
        in_specs=[
            x_spec,
            x_spec if paired else pl.BlockSpec((8, model), lambda j: (0, 0)),
            pl.BlockSpec((model, width), lambda j: (0, j)),
            pl.BlockSpec((model, width), lambda j: (0, count + j)),
            pl.BlockSpec((4, width), lambda j: (0, j)),
            pl.BlockSpec((width // group, group, 4 * group), lambda j: (j, 0, 0)),
            pl.BlockSpec((2, width), lambda j: (0, j)),
        ],
        out_specs=pl.BlockSpec((length, width), lambda j: (0, j)),
        scratch_shapes=[f32((length + 16, width)), f32((length, width))]
        + [f32((width // group, length, group)) for i in range(4)],
        compiler_params=pltpu.CompilerParams(vmem_limit_bytes=VMEM_BYTES),
        cost_estimate=pl.CostEstimate(
            flops=4 * length * model * channels + 16 * length * group * channels * 8,
            bytes_accessed=2 * (length * model + 2 * model * channels + length * channels),
            transcendentals=12 * length * channels,
        ),
    )(x, y, weights, weights, conv_weight, gates, coef)


def ffn_kernel(x_ref, gate_ref, up_ref, down_ref, out_ref, total):
    step = pl.program_id(0)
    gate = jnp.dot(x_ref[...], gate_ref[...], preferred_element_type=jnp.float32)
    up = jnp.dot(x_ref[...], up_ref[...], preferred_element_type=jnp.float32)
    hidden = (jax.nn.silu(gate) * up).astype(jnp.bfloat16)
    partial = lax.dot_general(
        hidden, down_ref[...], (((1,), (1,)), ((), ())), preferred_element_type=jnp.float32
    )

    @pl.when(step == 0)
    def _():
        total[...] = partial

    @pl.when(step > 0)
    def _():
        total[...] += partial

    @pl.when(step == pl.num_programs(0) - 1)
    def _():
        out_ref[...] = total[...].astype(jnp.bfloat16)


def ffn(x, weights):
    rows, model = x.shape
    units = weights.shape[1] // 3
    width = 256 if units % 256 == 0 else 128
    count = units // width
    return pl.pallas_call(
        ffn_kernel,
        grid=(count,),
        out_shape=jax.ShapeDtypeStruct((rows, model), jnp.bfloat16),
        in_specs=[
            pl.BlockSpec((rows, model), lambda j: (0, 0)),
            pl.BlockSpec((model, width), lambda j: (0, j)),
            pl.BlockSpec((model, width), lambda j: (0, count + j)),
            pl.BlockSpec((model, width), lambda j: (0, 2 * count + j)),
        ],
        out_specs=pl.BlockSpec((rows, model), lambda j: (0, 0)),
        scratch_shapes=[pltpu.VMEM((rows, model), jnp.float32)],
        compiler_params=pltpu.CompilerParams(vmem_limit_bytes=VMEM_BYTES),
        cost_estimate=pl.CostEstimate(
            flops=6 * rows * model * units,
            bytes_accessed=2 * (2 * rows * model + 3 * model * units),
            transcendentals=rows * units,
        ),
    )(x, weights, weights, weights)


def ring_chip(place, chips):
    half = chips // 2
    turned = place // half
    row = place * (1 - turned) + (chips - 1 - place) * turned
    return row * 2 + turned


def ring_kernel(
    size, shard_ref, x_ref, out_ref, other_ref, own_sem, send, recv, near_send, near_recv, swap_sem
):
    chips = size // 2
    me = lax.axis_index("fs")
    core = me % 2
    turned = (me // 2) % 2
    row = me // 4
    place = row * (1 - turned) + (chips - 1 - row) * turned
    partner = me + 1 - 2 * core
    after = ring_chip((place + 1) % chips, chips) * 2 + core
    before = ring_chip((place + chips - 1) % chips, chips) * 2 + core
    targets = ({"fs": after}, {"fs": before})
    partner = {"fs": partner}
    column = lax.axis_index("tp")
    across = {"tp": 1 - column}

    barrier = pltpu.get_barrier_semaphore()
    for device in (*targets, partner, across):
        pl.semaphore_signal(
            barrier, inc=1, device_id=device, device_id_type=pl.DeviceIdType.MESH
        )
    pl.semaphore_wait(barrier, 4)

    depth = shard_ref.shape[0]
    piece_rows = depth // (2 * PIECES)

    def remote(src, dst, sent, landed, device):
        copy = pltpu.make_async_remote_copy(
            src_ref=src,
            dst_ref=dst,
            send_sem=sent,
            recv_sem=landed,
            device_id=device,
            device_id_type=pl.DeviceIdType.MESH,
        )
        copy.start()
        return copy

    def rows_of(origin, at):
        start = pl.multiple_of(origin * depth + at * piece_rows, piece_rows)
        return out_ref.at[pl.ds(start, piece_rows), :]

    moving = []
    for at in range(2 * PIECES):
        moving.append(
            remote(
                shard_ref.at[pl.ds(at * piece_rows, piece_rows), :],
                rows_of(me, at),
                send.at[at, 0],
                recv.at[at, 0],
                targets[at % 2],
            )
        )
    waiting = list(moving)
    near = [remote(x_ref, other_ref, swap_sem.at[0], swap_sem.at[1], across)]
    mine = out_ref.at[pl.ds(pl.multiple_of(me * depth, depth), depth), :]
    near.append(remote(shard_ref, mine, near_send.at[0, 0], near_recv.at[0, 0], partner))
    own = pltpu.make_async_copy(shard_ref, mine, own_sem)
    own.start()
    for step in range(chips - 1):
        for at in range(2 * PIECES):
            moving[at].wait_recv()
            back = step + 1 if at % 2 == 0 else chips - 1 - step
            origin = ring_chip((place + chips - back) % chips, chips) * 2 + core
            piece = rows_of(origin, at)
            if step < chips - 2:
                moving[at] = remote(
                    piece,
                    piece,
                    send.at[at, step + 1],
                    recv.at[at, step + 1],
                    targets[at % 2],
                )
                waiting.append(moving[at])
            near.append(
                remote(
                    piece,
                    piece,
                    near_send.at[at, step + 1],
                    near_recv.at[at, step + 1],
                    partner,
                )
            )
    for copy in waiting:
        copy.wait_send()
    for copy in near:
        copy.wait()
    own.wait()


def ring_gather(shard, x, size):
    rows, width = shard.shape
    chips = size // 2
    dma = pltpu.SemaphoreType.DMA
    return pl.pallas_call(
        functools.partial(ring_kernel, size),
        out_shape=(
            jax.ShapeDtypeStruct((rows * size, width), shard.dtype),
            jax.ShapeDtypeStruct(x.shape, x.dtype),
        ),
        in_specs=[
            pl.BlockSpec(memory_space=pltpu.VMEM),
            pl.BlockSpec(memory_space=pl.ANY),
        ],
        out_specs=(pl.BlockSpec(memory_space=pl.ANY), pl.BlockSpec(memory_space=pl.ANY)),
        scratch_shapes=[
            dma,
            dma((2 * PIECES, chips)),
            dma((2 * PIECES, chips)),
            dma((2 * PIECES, chips)),
            dma((2 * PIECES, chips)),
            dma((2,)),
        ],
        compiler_params=pltpu.CompilerParams(collective_id=0, has_side_effects=True),
        cost_estimate=pl.CostEstimate(
            flops=1 << 32, bytes_accessed=2 * rows * size * width, transcendentals=0
        ),
    )(shard, x)


def swap(values):
    return lax.ppermute(values, "tp", [(0, 1), (1, 0)])


def matmul_t(rows, weight_t):
    return lax.dot_general(
        rows, weight_t, (((1,), (1,)), ((), ())), preferred_element_type=jnp.float32
    )


def per_device(
    pair,
    tokens,
    pre_mix_gain,
    post_mix_gain,
    pre_ffn_gain,
    post_ffn_gain,
    w_branch,
    w_gelu,
    conv_weight,
    w_rec,
    w_inp,
    decay,
    out_weight_t,
    w_gate,
    w_up,
    down_weight_t,
):
    own_rows = tokens.shape[0]
    channels = conv_weight.shape[1]
    place = lax.axis_index("tp")
    mix_shard = jnp.concatenate([w_branch, w_gelu, out_weight_t], axis=1)
    ffn_shard = jnp.concatenate([w_gate, w_up, down_weight_t], axis=1)
    stream = tokens.astype(jnp.float32)
    normed_in = normed(stream, pre_mix_gain).astype(jnp.bfloat16)
    if pair:
        fs_size = lax.axis_size("fs")
        mix_all, other = ring_gather(mix_shard, normed_in, fs_size)
        ffn_shard, mix_all, other = lax.optimization_barrier((ffn_shard, mix_all, other))
        sequence = (normed_in, other)
    else:
        mix_all = lax.all_gather(mix_shard, "fs", axis=0, tiled=True)
        whole = lax.all_gather(normed_in, "tp", axis=0, tiled=True)
        sequence = (whole, whole)
    ffn_all = lax.all_gather(ffn_shard, "fs", axis=0, tiled=True)
    out_own = mix_all[:, 2 * channels :]
    if pair:
        core = lax.axis_index("fs") % 2
        span = out_own.shape[0] // 2
        partners = [(i, i + 1 - 2 * (i % 2)) for i in range(fs_size)]
        crossed = swap(lax.dynamic_slice_in_dim(out_own, core * span, span, 0))
    hidden = mixer(pair, *sequence, mix_all, conv_weight, w_rec, w_inp, decay)
    if pair:
        crossed, hidden = lax.optimization_barrier((crossed, hidden))
        shared = lax.ppermute(crossed, "fs", partners)
        out_other = (
            jnp.where(core == 0, crossed, shared),
            jnp.where(core == 0, shared, crossed),
        )
        away = lax.dynamic_slice_in_dim(hidden, (1 - place) * own_rows, own_rows, 0)
        kept = lax.dynamic_slice_in_dim(hidden, place * own_rows, own_rows, 0)
        came = swap(away)
        far = jnp.concatenate(out_other, axis=0)
        mixer_sum = matmul_t(kept, out_own) + matmul_t(came, far)
    else:
        own_hidden = lax.all_to_all(hidden, "tp", split_axis=0, concat_axis=1, tiled=True)
        out_whole = lax.all_gather(out_own, "tp", axis=1, tiled=True)
        mixer_sum = matmul_t(own_hidden, out_whole)
    residual = (stream + normed(mixer_sum, post_mix_gain)).astype(jnp.bfloat16)
    middle = residual.astype(jnp.float32)
    normed_mid = normed(middle, pre_ffn_gain).astype(jnp.bfloat16)
    if pair:
        pieces = 2
        size = own_rows // pieces
        away_rows = [swap(normed_mid[i * size : (i + 1) * size]) for i in range(pieces)]
        back = [swap(ffn(rows, ffn_all)) for rows in away_rows]
        own_part = ffn(normed_mid, ffn_all).astype(jnp.float32)
        ffn_sum = own_part + jnp.concatenate(back, axis=0).astype(jnp.float32)
    else:
        all_mid = lax.all_gather(normed_mid, "tp", axis=0, tiled=True)
        ffn_sum = lax.psum_scatter(
            ffn(all_mid, ffn_all), "tp", scatter_dimension=0, tiled=True
        ).astype(jnp.float32)
    return (middle + normed(ffn_sum, post_ffn_gain)).astype(jnp.bfloat16)


def solution(mesh):
    return jax.shard_map(
        functools.partial(per_device, mesh.shape["tp"] == 2),
        mesh=mesh,
        in_specs=(
            P(("fs", "tp"), None),
            P(),
            P(),
            P(),
            P(),
            P("fs", "tp"),
            P("fs", "tp"),
            P(None, "tp"),
            P(None, "tp", None, None),
            P(None, "tp", None, None),
            P(None, "tp"),
            P("fs", "tp"),
            P("fs", "tp"),
            P("fs", "tp"),
            P("fs", "tp"),
        ),
        out_specs=P(("fs", "tp"), None),
        check_vma=False,
    )
```

```python
import functools

import jax
import jax.numpy as jnp
from jax import lax
from jax.experimental import pallas as pl
from jax.experimental.pallas import tpu as pltpu
from jax.sharding import PartitionSpec as P

EPS = 1e-06
SEGMENTS = 8
PIECES = 4
ROW_BLOCK = 64
VMEM_BYTES = 60 * 1024 * 1024


def normed(values, gain):
    factor = lax.rsqrt(jnp.mean(values * values, axis=-1, keepdims=True) + EPS)
    return values * factor * gain


def one_minus_exp(y, exp_y):
    series = 1.0 + y * (1.0 / 8.0)
    for order in (7, 6, 5, 4, 3, 2):
        series = 1.0 + y * (1.0 / order) * series
    return jnp.where(y > -0.5, -y * series, 1.0 - exp_y)


def mixer_kernel(
    paired, x_ref, y_ref, wb_ref, wg_ref, conv_ref, gates_ref, coef_ref, out_ref, pad, gel, a0, u0, a1, u1
):
    length, width = out_ref.shape
    group = gates_ref.shape[1]
    rows = 256
    pad[0:8, :] = jnp.zeros((8, width), jnp.float32)
    pad[8 + length : 16 + length, :] = jnp.zeros((8, width), jnp.float32)
    if paired:
        own_start = lax.axis_index("tp") * x_ref.shape[0]
        sources = ((x_ref, own_start), (y_ref, x_ref.shape[0] - own_start))
    else:
        sources = ((x_ref, 0),)
    for source, base in sources:
        for start in range(0, source.shape[0], rows):
            piece = source[start : start + rows, :]
            branch = jnp.dot(piece, wb_ref[...], preferred_element_type=jnp.float32)
            gelu_in = jnp.dot(piece, wg_ref[...], preferred_element_type=jnp.float32)
            at = pl.multiple_of(base + start, rows)
            pad[pl.ds(8 + at, rows), :] = branch.astype(jnp.bfloat16).astype(jnp.float32)
            gel[pl.ds(at, rows), :] = jax.nn.gelu(
                gelu_in.astype(jnp.bfloat16).astype(jnp.float32)
            )

    for part in range(width // group):
        cols = slice(part * group, (part + 1) * group)
        taps = conv_ref[:, cols].astype(jnp.float32)
        coef = coef_ref[:, cols]
        for start in range(0, length, rows):
            summed = taps[0:1] * pad[6 + start : 6 + start + rows, cols]
            for j in range(1, 4):
                summed = summed + taps[j : j + 1] * pad[6 + j + start : 6 + j + start + rows, cols]
            conv = summed.astype(jnp.bfloat16)
            wide = conv.astype(jnp.float32)
            for d, (a_ref, u_ref) in enumerate(((a0, u0), (a1, u1))):
                gate = jnp.dot(
                    conv,
                    gates_ref[part, :, 2 * d * group : 2 * (d + 1) * group],
                    preferred_element_type=jnp.float32,
                )
                rate = jax.nn.sigmoid(gate[:, :group])
                inflow = jax.nn.sigmoid(gate[:, group:])
                log_retain = rate * coef[d : d + 1]
                retain = jnp.exp(log_retain)
                left = one_minus_exp(2.0 * log_retain, retain * retain)
                a_ref[part, start : start + rows, :] = retain
                u_ref[part, start : start + rows, :] = jnp.sqrt(left) * inflow * wide

    steps = length // SEGMENTS

    def step(t, carry):
        out = []
        for (state, decayed), (a_ref, u_ref), at in (
            (carry[0], (a0, u0), t),
            (carry[1], (a1, u1), steps - 1 - t),
        ):
            where = pl.ds(at, SEGMENTS, stride=steps)
            nstate, ndecayed = [], []
            for c in range(n):
                retain = a_ref[c, where, :]
                h = retain * state[c] + u_ref[c, where, :]
                p = retain * decayed[c]
                u_ref[c, where, :] = h
                a_ref[c, where, :] = p
                nstate.append(h)
                ndecayed.append(p)
            out.append((tuple(nstate), tuple(ndecayed)))
        return tuple(out)

    n = width // group
    zero = tuple(jnp.zeros((SEGMENTS, group), jnp.float32) for c in range(n))
    one = tuple(jnp.ones((SEGMENTS, group), jnp.float32) for c in range(n))
    ended = lax.fori_loop(0, steps, step, ((zero, one), (zero, one)), unroll=8)
    for c in range(n):
        lanes = slice(c * group, (c + 1) * group)
        blank = jnp.zeros((1, group), jnp.float32)
        entry = [[None] * SEGMENTS, [None] * SEGMENTS]
        for d, order in ((0, range(SEGMENTS)), (1, range(SEGMENTS - 1, -1, -1))):
            carry = blank
            for s in order:
                entry[d][s] = carry
                carry = ended[d][0][c][s : s + 1] + ended[d][1][c][s : s + 1] * carry
        for s in range(SEGMENTS):
            span = slice(s * steps, (s + 1) * steps)
            forward = u0[c, span, :] + a0[c, span, :] * entry[0][s]
            backward = u1[c, span, :] + a1[c, span, :] * entry[1][s]
            out_ref[span, lanes] = (gel[span, lanes] * (forward + backward)).astype(jnp.bfloat16)


def mixer(paired, x, y, weights, conv_weight, w_rec, w_inp, decay):
    length, model = x.shape
    x_spec = pl.BlockSpec((length, model), lambda j: (0, 0))
    length = 2 * length if paired else length
    channels = conv_weight.shape[1]
    group = w_rec.shape[2]
    width = min(256, channels)
    count = channels // width
    gates = jnp.concatenate([w_rec[0], w_inp[0], w_rec[1], w_inp[1]], axis=-1)
    coef = -8.0 * jax.nn.softplus(-decay)
    f32 = functools.partial(pltpu.VMEM, dtype=jnp.float32)
    return pl.pallas_call(
        functools.partial(mixer_kernel, paired),
        grid=(count,),
        out_shape=jax.ShapeDtypeStruct((length, channels), jnp.bfloat16),
        in_specs=[
            x_spec,
            x_spec if paired else pl.BlockSpec((8, model), lambda j: (0, 0)),
            pl.BlockSpec((model, width), lambda j: (0, j)),
            pl.BlockSpec((model, width), lambda j: (0, count + j)),
            pl.BlockSpec((4, width), lambda j: (0, j)),
            pl.BlockSpec((width // group, group, 4 * group), lambda j: (j, 0, 0)),
            pl.BlockSpec((2, width), lambda j: (0, j)),
        ],
        out_specs=pl.BlockSpec((length, width), lambda j: (0, j)),
        scratch_shapes=[f32((length + 16, width)), f32((length, width))]
        + [f32((width // group, length, group)) for i in range(4)],
        compiler_params=pltpu.CompilerParams(vmem_limit_bytes=VMEM_BYTES),
        cost_estimate=pl.CostEstimate(
            flops=4 * length * model * channels + 16 * length * group * channels * 8,
            bytes_accessed=2 * (length * model + 2 * model * channels + length * channels),
            transcendentals=12 * length * channels,
        ),
    )(x, y, weights, weights, conv_weight, gates, coef)


def ffn_kernel(x_ref, gate_ref, up_ref, down_ref, out_ref, total):
    step = pl.program_id(0)
    gate = jnp.dot(x_ref[...], gate_ref[...], preferred_element_type=jnp.float32)
    up = jnp.dot(x_ref[...], up_ref[...], preferred_element_type=jnp.float32)
    hidden = (jax.nn.silu(gate) * up).astype(jnp.bfloat16)
    partial = lax.dot_general(
        hidden, down_ref[...], (((1,), (1,)), ((), ())), preferred_element_type=jnp.float32
    )

    @pl.when(step == 0)
    def _():
        total[...] = partial

    @pl.when(step > 0)
    def _():
        total[...] += partial

    @pl.when(step == pl.num_programs(0) - 1)
    def _():
        out_ref[...] = total[...].astype(jnp.bfloat16)


def ffn(x, weights):
    rows, model = x.shape
    units = weights.shape[1] // 3
    width = 256 if units % 256 == 0 else 128
    count = units // width
    return pl.pallas_call(
        ffn_kernel,
        grid=(count,),
        out_shape=jax.ShapeDtypeStruct((rows, model), jnp.bfloat16),
        in_specs=[
            pl.BlockSpec((rows, model), lambda j: (0, 0)),
            pl.BlockSpec((model, width), lambda j: (0, j)),
            pl.BlockSpec((model, width), lambda j: (0, count + j)),
            pl.BlockSpec((model, width), lambda j: (0, 2 * count + j)),
        ],
        out_specs=pl.BlockSpec((rows, model), lambda j: (0, 0)),
        scratch_shapes=[pltpu.VMEM((rows, model), jnp.float32)],
        compiler_params=pltpu.CompilerParams(vmem_limit_bytes=VMEM_BYTES),
        cost_estimate=pl.CostEstimate(
            flops=6 * rows * model * units,
            bytes_accessed=2 * (2 * rows * model + 3 * model * units),
            transcendentals=rows * units,
        ),
    )(x, weights, weights, weights)


def ring_chip(place, chips):
    half = chips // 2
    turned = place // half
    row = place * (1 - turned) + (chips - 1 - place) * turned
    return row * 2 + turned


def ring_kernel(
    size, shard_ref, x_ref, out_ref, other_ref, own_sem, send, recv, near_send, near_recv, swap_sem
):
    chips = size // 2
    me = lax.axis_index("fs")
    core = me % 2
    turned = (me // 2) % 2
    row = me // 4
    place = row * (1 - turned) + (chips - 1 - row) * turned
    partner = me + 1 - 2 * core
    after = ring_chip((place + 1) % chips, chips) * 2 + core
    before = ring_chip((place + chips - 1) % chips, chips) * 2 + core
    targets = ({"fs": after}, {"fs": before})
    partner = {"fs": partner}
    column = lax.axis_index("tp")
    across = {"tp": 1 - column}

    barrier = pltpu.get_barrier_semaphore()
    for device in (*targets, partner, across):
        pl.semaphore_signal(
            barrier, inc=1, device_id=device, device_id_type=pl.DeviceIdType.MESH
        )
    pl.semaphore_wait(barrier, 4)

    depth = shard_ref.shape[0]
    piece_rows = depth // (2 * PIECES)

    def remote(src, dst, sent, landed, device):
        copy = pltpu.make_async_remote_copy(
            src_ref=src,
            dst_ref=dst,
            send_sem=sent,
            recv_sem=landed,
            device_id=device,
            device_id_type=pl.DeviceIdType.MESH,
        )
        copy.start()
        return copy

    def rows_of(origin, at):
        start = pl.multiple_of(origin * depth + at * piece_rows, piece_rows)
        return out_ref.at[pl.ds(start, piece_rows), :]

    moving = []
    for at in range(2 * PIECES):
        moving.append(
            remote(
                shard_ref.at[pl.ds(at * piece_rows, piece_rows), :],
                rows_of(me, at),
                send.at[at, 0],
                recv.at[at, 0],
                targets[at % 2],
            )
        )
    waiting = list(moving)
    near = [remote(x_ref, other_ref, swap_sem.at[0], swap_sem.at[1], across)]
    mine = out_ref.at[pl.ds(pl.multiple_of(me * depth, depth), depth), :]
    near.append(remote(shard_ref, mine, near_send.at[0, 0], near_recv.at[0, 0], partner))
    own = pltpu.make_async_copy(shard_ref, mine, own_sem)
    own.start()
    for step in range(chips - 1):
        for at in range(2 * PIECES):
            moving[at].wait_recv()
            back = step + 1 if at % 2 == 0 else chips - 1 - step
            origin = ring_chip((place + chips - back) % chips, chips) * 2 + core
            piece = rows_of(origin, at)
            if step < chips - 2:
                moving[at] = remote(
                    piece,
                    piece,
                    send.at[at, step + 1],
                    recv.at[at, step + 1],
                    targets[at % 2],
                )
                waiting.append(moving[at])
            near.append(
                remote(
                    piece,
                    piece,
                    near_send.at[at, step + 1],
                    near_recv.at[at, step + 1],
                    partner,
                )
            )
    for copy in waiting:
        copy.wait_send()
    for copy in near:
        copy.wait()
    own.wait()


def ring_gather(shard, x, size):
    rows, width = shard.shape
    chips = size // 2
    dma = pltpu.SemaphoreType.DMA
    return pl.pallas_call(
        functools.partial(ring_kernel, size),
        out_shape=(
            jax.ShapeDtypeStruct((rows * size, width), shard.dtype),
            jax.ShapeDtypeStruct(x.shape, x.dtype),
        ),
        in_specs=[
            pl.BlockSpec(memory_space=pltpu.VMEM),
            pl.BlockSpec(memory_space=pl.ANY),
        ],
        out_specs=(pl.BlockSpec(memory_space=pl.ANY), pl.BlockSpec(memory_space=pl.ANY)),
        scratch_shapes=[
            dma,
            dma((2 * PIECES, chips)),
            dma((2 * PIECES, chips)),
            dma((2 * PIECES, chips)),
            dma((2 * PIECES, chips)),
            dma((2,)),
        ],
        compiler_params=pltpu.CompilerParams(collective_id=0, has_side_effects=True),
        cost_estimate=pl.CostEstimate(
            flops=1 << 32, bytes_accessed=2 * rows * size * width, transcendentals=0
        ),
    )(shard, x)


def finish_kernel(middle_ref, own_ref, back_ref, gain_ref, *rest):
    out_ref = rest[-1]
    ffn_sum = own_ref[...].astype(jnp.float32) + back_ref[...].astype(jnp.float32)
    out_ref[...] = (
        middle_ref[...].astype(jnp.float32) + normed(ffn_sum, gain_ref[...])
    ).astype(jnp.bfloat16)


def finish(middle, own, back, gain, start, done):
    model = middle.shape[1]
    rows = ROW_BLOCK
    first = start // rows
    placed = pl.BlockSpec((rows, model), lambda i: (first + i, 0))
    operands = [middle, own, back, gain.reshape(1, model)]
    specs = [
        placed,
        placed,
        pl.BlockSpec((rows, model), lambda i: (i, 0)),
        pl.BlockSpec((1, model), lambda i: (0, 0)),
    ]
    aliases = {}
    if done is not None:
        aliases = {len(operands): 0}
        operands.append(done)
        specs.append(pl.BlockSpec(memory_space=pl.ANY))
    return pl.pallas_call(
        finish_kernel,
        grid=(back.shape[0] // rows,),
        out_shape=jax.ShapeDtypeStruct(middle.shape, jnp.bfloat16),
        in_specs=specs,
        out_specs=placed,
        input_output_aliases=aliases,
        cost_estimate=pl.CostEstimate(
            flops=8 * back.size, bytes_accessed=8 * back.size, transcendentals=0
        ),
    )(*operands)


def swap(values):
    return lax.ppermute(values, "tp", [(0, 1), (1, 0)])


def matmul_t(rows, weight_t):
    return lax.dot_general(
        rows, weight_t, (((1,), (1,)), ((), ())), preferred_element_type=jnp.float32
    )


def per_device(
    pair,
    tokens,
    pre_mix_gain,
    post_mix_gain,
    pre_ffn_gain,
    post_ffn_gain,
    w_branch,
    w_gelu,
    conv_weight,
    w_rec,
    w_inp,
    decay,
    out_weight_t,
    w_gate,
    w_up,
    down_weight_t,
):
    own_rows = tokens.shape[0]
    channels = conv_weight.shape[1]
    place = lax.axis_index("tp")
    mix_shard = jnp.concatenate([w_branch, w_gelu, out_weight_t], axis=1)
    ffn_shard = jnp.concatenate([w_gate, w_up, down_weight_t], axis=1)
    stream = tokens.astype(jnp.float32)
    normed_in = normed(stream, pre_mix_gain).astype(jnp.bfloat16)
    if pair:
        fs_size = lax.axis_size("fs")
        mix_all, other = ring_gather(mix_shard, normed_in, fs_size)
        ffn_shard, mix_all, other = lax.optimization_barrier((ffn_shard, mix_all, other))
        sequence = (normed_in, other)
    else:
        mix_all = lax.all_gather(mix_shard, "fs", axis=0, tiled=True)
        whole = lax.all_gather(normed_in, "tp", axis=0, tiled=True)
        sequence = (whole, whole)
    ffn_all = lax.all_gather(ffn_shard, "fs", axis=0, tiled=True)
    out_own = mix_all[:, 2 * channels :]
    if pair:
        core = lax.axis_index("fs") % 2
        span = out_own.shape[0] // 2
        partners = [(i, i + 1 - 2 * (i % 2)) for i in range(fs_size)]
        crossed = swap(lax.dynamic_slice_in_dim(out_own, core * span, span, 0))
    hidden = mixer(pair, *sequence, mix_all, conv_weight, w_rec, w_inp, decay)
    if pair:
        crossed, hidden = lax.optimization_barrier((crossed, hidden))
        shared = lax.ppermute(crossed, "fs", partners)
        out_other = (
            jnp.where(core == 0, crossed, shared),
            jnp.where(core == 0, shared, crossed),
        )
        away = lax.dynamic_slice_in_dim(hidden, (1 - place) * own_rows, own_rows, 0)
        kept = lax.dynamic_slice_in_dim(hidden, place * own_rows, own_rows, 0)
        came = swap(away)
        far = jnp.concatenate(out_other, axis=0)
        mixer_sum = matmul_t(kept, out_own) + matmul_t(came, far)
    else:
        own_hidden = lax.all_to_all(hidden, "tp", split_axis=0, concat_axis=1, tiled=True)
        out_whole = lax.all_gather(out_own, "tp", axis=1, tiled=True)
        mixer_sum = matmul_t(own_hidden, out_whole)
    residual = (stream + normed(mixer_sum, post_mix_gain)).astype(jnp.bfloat16)
    middle = residual.astype(jnp.float32)
    normed_mid = normed(middle, pre_ffn_gain).astype(jnp.bfloat16)
    if pair:
        blocks = own_rows // ROW_BLOCK
        cuts = [0, blocks // 4, blocks // 4 + 3 * blocks // 8, blocks]
        spans = [(i * ROW_BLOCK, j * ROW_BLOCK) for i, j in zip(cuts, cuts[1:])]
        away_rows, partials = [], []
        for start, end in spans:
            rows = normed_mid[start:end]
            if away_rows:
                rows, away_rows[-1] = lax.optimization_barrier((rows, away_rows[-1]))
            away_rows.append(swap(rows))
        for rows in away_rows:
            if partials:
                rows, partials[-1] = lax.optimization_barrier((rows, partials[-1]))
            partials.append(ffn(rows, ffn_all))
        normed_mid, partials[-1] = lax.optimization_barrier((normed_mid, partials[-1]))
        back = [swap(partial) for partial in partials]
        own_part = ffn(normed_mid, ffn_all)
        done = None
        for (start, end), came in zip(spans, back):
            done = finish(residual, own_part, came, post_ffn_gain, start, done)
        return done
    else:
        all_mid = lax.all_gather(normed_mid, "tp", axis=0, tiled=True)
        ffn_sum = lax.psum_scatter(
            ffn(all_mid, ffn_all), "tp", scatter_dimension=0, tiled=True
        ).astype(jnp.float32)
    return (middle + normed(ffn_sum, post_ffn_gain)).astype(jnp.bfloat16)


def solution(mesh):
    return jax.shard_map(
        functools.partial(per_device, mesh.shape["tp"] == 2),
        mesh=mesh,
        in_specs=(
            P(("fs", "tp"), None),
            P(),
            P(),
            P(),
            P(),
            P("fs", "tp"),
            P("fs", "tp"),
            P(None, "tp"),
            P(None, "tp", None, None),
            P(None, "tp", None, None),
            P(None, "tp"),
            P("fs", "tp"),
            P("fs", "tp"),
            P("fs", "tp"),
            P("fs", "tp"),
        ),
        out_specs=P(("fs", "tp"), None),
        check_vma=False,
    )
```
